256 devices in a mesh: kv: 16 (over y, x), tp: 16 (over z, core).
Axes of the slice: x: 4, y: 4, z: 8, core: 2. Of those that a mesh axis runs over, the one named last changes fastest.
Arguments:
- tokens: bfloat16 [1024, 4096], P('tp', 'kv'), may hold values from -19 to 19, as said below
- lengths: int32 [1024], P('kv'), may hold values from 1 to 16384, 4194304 in all
- state_block: float32 [1024, 64, 2048], P('kv', None, 'tp'), may hold values from -6 to 6
- cached_keys: bfloat16 [1024, 128, 2048], P('kv', None, 'tp'), may hold values from -0.75 to 0.75
- cached_values: bfloat16 [1024, 128, 2048], P('kv', None, 'tp'), may hold values from -6 to 6
- query_weight: bfloat16 [4096, 2048], P('kv', 'tp'), may hold values from -0.09375 to 0.09375
- key_weight: bfloat16 [4096, 2048], P('kv', 'tp'), may hold values from -0.09375 to 0.09375
- value_weight: bfloat16 [4096, 2048], P('kv', 'tp'), may hold values from -0.09375 to 0.09375
- gate_weight: bfloat16 [4096, 2048], P('kv', 'tp'), may hold values from -0.09375 to 0.09375
- decay_rate: float32 [32], P('tp'), may hold values from 0.0005 to 0.05
- head_gain: float32 [2048], P('tp'), may hold values from 0.1 to 1.9
- out_weight: bfloat16 [2048, 4096], P('tp', 'kv'), may hold values from -0.125 to 0.125
- mixer_gain: float32 [4096], P('kv'), may hold values from 0.1 to 1.9
- up_weight: bfloat16 [4096, 16384], P('kv', 'tp'), may hold values from -0.09375 to 0.09375
- down_weight: bfloat16 [16384, 4096], P('tp', 'kv'), may hold values from -0.046875 to 0.046875
- final_gain: float32 [4096], P('kv'), may hold values from 0.1 to 1.9
Outputs:
- next_rows: bfloat16 [1024, 4096], P('tp', 'kv')
The draws below stay inside these ranges and needn't reach their ends.
Inputs may be any that keep to these rules, and one draw needn't show every extreme that they name: `tokens`: the rows' column groups have scales that differ between groups.
All inputs are finite; a program needn't handle non-finite values. No bound on the sum of `lengths` on one device may be relied on, other than what follows from the above.
Results may differ from the reference program's by a relative error of at most 0.0095.
Values may be sent and summed in bfloat16 or wider, within the bound.
No kernel may reach another device: no remote copies, remote signals or barrier semaphores. Data moves between devices by JAX's collectives and lax.ppermute only.
A program may use at most 64 MiB of HBM per device.

```python
import math
import jax
import jax.numpy as jnp
import numpy as np
from jax import lax

D = 4096
HEADS = 32
HDIM = 64
FF = 16384
SEQ_DEV = 64
BLK = 128
LEN_MOST = 16384
RW = 2048
ROWS = 1024
LEN_TOTAL = 4194304


def draw_tokens(key, part):
    base, group_key = jax.random.split(jax.random.fold_in(key, 11))
    groups = max(D // 256, 1)
    scales = jnp.exp(jax.random.uniform(group_key, (groups,), jnp.float32, -1.1, 1.1))
    column = jnp.repeat(scales, D // groups, total_repeat_length=D)
    values = jnp.clip(jax.random.normal(base, (ROWS, D), jnp.float32), -6.0, 6.0)
    return (values * column[None, :]).astype(jnp.bfloat16)


def levels(stream_key, dims, cuts, smallest, top_value):
    level, own = 1.0, jax.random.fold_in(stream_key, 6)
    for dim, shards_of in cuts:
        heights = jnp.exp(jax.random.uniform(jax.random.fold_in(own, dim), (shards_of,), jnp.float32, smallest / len(cuts), top_value / len(cuts)))
        level = level * jnp.repeat(heights, dims[dim] // shards_of).reshape([-1 if axis == dim else 1 for axis in range(len(dims))])
    return level


def profile(number_of, total, most, lean):
    weights = [(1 << 20) // math.isqrt(rank ** lean) + 1 for rank in range(2, number_of + 1)]
    spare, counts = total - most - (number_of - 1), [1] * (number_of - 1)
    while spare > 0:
        candidates = [i for i in range(number_of - 1) if counts[i] < most]
        mass, remaining = sum([weights[i] for i in candidates]), spare
        for i in candidates:
            extra = min(most - counts[i], max(1, remaining * weights[i] // mass), spare)
            counts[i] = counts[i] + extra
            spare = spare - extra
    return np.array([most] + counts)


def ragged(key, number_of, total, bound, skew):
    if number_of == 2:
        one = jax.random.randint(key, (), max(1, total - bound), min(bound, total - 1) + 1)
        return jnp.stack([one, total - one])
    tallies = jnp.asarray(profile(number_of, total, bound, skew), jnp.int32)
    pairs = (number_of - 1) // 2
    giver, receiver = tallies[1:1 + 2 * pairs:2], tallies[2:2 + 2 * pairs:2]
    slack = jnp.minimum(giver - 1, bound - receiver)
    passed = jax.random.randint(jax.random.fold_in(key, 1), (pairs,), 0, 1 << 20) % (slack + 1)
    tallies = tallies.at[1:1 + 2 * pairs:2].set(giver - passed).at[2:2 + 2 * pairs:2].set(receiver + passed)
    return tallies[jax.random.permutation(jax.random.fold_in(key, 2), number_of)]


def bell_draw(rng, shape, scale, bound, cuts=(), kind=jnp.bfloat16):
    level = levels(rng, shape, cuts, -0.22, 0.18) if cuts else 1.0
    entries = jax.random.normal(rng, shape, jnp.float32) * scale * level
    return jnp.minimum(jnp.maximum(entries, -bound), bound).astype(kind)


def setup_inputs(seed: int = 0) -> dict:
    seeds = jax.random.split(jax.random.key(seed), 17)
    tokens = draw_tokens(jax.random.fold_in(seeds[16], 71), 0)
    lengths = ragged(seeds[1], ROWS, LEN_TOTAL, LEN_MOST, 2).astype(jnp.int32)
    state_block = bell_draw(seeds[2], (ROWS, HDIM, RW), 1.0, 6.0, ((0, 16), (2, 16)), jnp.float32)
    cached_keys = bell_draw(seeds[3], (ROWS, BLK, RW), 0.125, 0.75, ((0, 16), (2, 16)))
    cached_values = bell_draw(seeds[4], (ROWS, BLK, RW), 1.0, 6.0, ((0, 16), (2, 16)))
    query_weight = bell_draw(seeds[5], (D, RW), D ** -0.5, 0.09375, ((0, 16), (1, 16)))
    key_weight = bell_draw(seeds[6], (D, RW), D ** -0.5, 0.09375, ((0, 16), (1, 16)))
    value_weight = bell_draw(seeds[7], (D, RW), D ** -0.5, 0.09375, ((0, 16), (1, 16)))
    gate_weight = bell_draw(seeds[8], (D, RW), D ** -0.5, 0.09375, ((0, 16), (1, 16)))
    decay_rate = jnp.clip(jnp.exp(math.log(0.05) - 4.6051702 * jax.random.uniform(seeds[9], (HEADS,), jnp.float32) ** levels(seeds[9], (HEADS,), ((0, 16),), -0.2, 0.2)), 0.0005, 0.05)
    head_gain = jnp.clip(1.0 + 0.18 * jax.random.normal(seeds[10], (RW,), jnp.float32), 0.1, 1.9)
    out_weight = bell_draw(seeds[11], (RW, D), RW ** -0.5, 0.125, ((0, 16), (1, 16)))
    mixer_gain = jnp.clip(1.0 + 0.18 * jax.random.normal(seeds[12], (D,), jnp.float32), 0.1, 1.9)
    up_weight = bell_draw(seeds[13], (D, FF), D ** -0.5, 0.09375, ((0, 16), (1, 16)))
    down_weight = bell_draw(seeds[14], (FF, D), FF ** -0.5, 0.046875, ((0, 16), (1, 16)))
    final_gain = jnp.clip(1.0 + 0.18 * jax.random.normal(seeds[15], (D,), jnp.float32), 0.1, 1.9)
    return {"tokens": tokens, "lengths": lengths, "state_block": state_block, "cached_keys": cached_keys, "cached_values": cached_values, "query_weight": query_weight, "key_weight": key_weight, "value_weight": value_weight, "gate_weight": gate_weight, "decay_rate": decay_rate, "head_gain": head_gain, "out_weight": out_weight, "mixer_gain": mixer_gain, "up_weight": up_weight, "down_weight": down_weight, "final_gain": final_gain}


ALPHA = 2.0 ** 0.5
EPS = 1e-05

def rotate(vectors, positions):
    half = vectors.shape[-1] // 2
    inverse = 10000.0 ** (-jnp.arange(half, dtype=jnp.float32) / half)
    angle = positions.astype(jnp.float32)[:, None] * inverse[None, :]
    cosine = jnp.cos(angle)[:, None, :]
    sine = jnp.sin(angle)[:, None, :]
    former, latter = (vectors[..., :half], vectors[..., half:])
    return jnp.concatenate([former * cosine - latter * sine, latter * cosine + former * sine], -1)

def layer_norm(values, gain):
    mean = lax.optimization_barrier(jnp.mean(values, 1, keepdims=True))
    centred = values - mean
    spread = lax.optimization_barrier(jnp.mean(centred * centred, 1, keepdims=True))
    return centred * lax.rsqrt(spread + EPS) * gain[None, :]

def retain(query, keyed, valued, gated, lengths, state, keys, values, rate, gain):
    count = query.shape[0]
    heads = rate.shape[0]
    q_rot = rotate(query.astype(jnp.float32).reshape(count, heads, HDIM), lengths).astype(jnp.bfloat16)
    k_rot = (rotate(keyed.astype(jnp.float32).reshape(count, heads, HDIM), lengths) * 0.125).astype(jnp.bfloat16)
    v_new = valued.astype(jnp.float32).reshape(count, heads, HDIM)
    cached_k = keys.astype(jnp.float32).reshape(count, BLK, heads, HDIM)
    cached_v = values.astype(jnp.float32).reshape(count, BLK, heads, HDIM)
    q_wide = q_rot.astype(jnp.float32)
    scores = jnp.einsum('shn,sihn->shi', q_wide, cached_k)
    offset = lengths % BLK
    slots = jnp.arange(BLK, dtype=jnp.int32)
    lag = jnp.maximum(offset[:, None] - slots[None, :], 0).astype(jnp.float32)
    live = (slots[None, :] < offset[:, None])[:, None, :]
    factor = jnp.where(live, jnp.exp(-rate[None, :, None] * lag[:, None, :]), 0.0)
    weights = (scores * factor).astype(jnp.bfloat16).astype(jnp.float32)
    own = lax.optimization_barrier(jnp.sum(q_wide * k_rot.astype(jnp.float32), -1)).astype(jnp.bfloat16).astype(jnp.float32)
    inner = jnp.einsum('shi,sihn->shn', weights, cached_v) + own[..., None] * v_new
    carried = jnp.exp(-rate[None, :] * (offset[:, None] + 1).astype(jnp.float32))
    cross = jnp.einsum('shk,skhv->shv', q_wide, state.reshape(count, HDIM, heads, HDIM), precision=lax.Precision.HIGHEST) * carried[..., None]
    retained = inner + cross
    mean = lax.optimization_barrier(jnp.mean(retained, -1, keepdims=True))
    centred = retained - mean
    spread = lax.optimization_barrier(jnp.mean(centred * centred, -1, keepdims=True))
    normed = centred * lax.rsqrt(spread + EPS) * gain.reshape(heads, HDIM)[None]
    gate_f = jax.nn.silu(gated.astype(jnp.float32).reshape(count, heads, HDIM))
    return (gate_f * normed).reshape(count, heads * HDIM).astype(jnp.bfloat16)

def reference(tokens, lengths, state_block, cached_keys, cached_values, query_weight, key_weight, value_weight, gate_weight, decay_rate, head_gain, out_weight, mixer_gain, up_weight, down_weight, final_gain):
    projected = [jnp.dot(tokens, weight, preferred_element_type=jnp.float32).astype(jnp.bfloat16) for weight in (query_weight, key_weight, value_weight, gate_weight)]
    blocks = ROWS // SEQ_DEV

    def split_rows(array):
        return array.reshape((blocks, SEQ_DEV) + array.shape[1:])

    def one_block(items):
        query, keyed, valued, gated, length_rows, state, keys, values = items
        return retain(query, keyed, valued, gated, length_rows, state, keys, values, decay_rate, head_gain)
    mixed = lax.map(one_block, tuple((split_rows(array) for array in projected + [lengths, state_block, cached_keys, cached_values])))
    mixed = mixed.reshape(ROWS, RW)
    branch = jnp.dot(mixed, out_weight, preferred_element_type=jnp.float32)
    hidden = layer_norm(ALPHA * tokens.astype(jnp.float32) + branch, mixer_gain).astype(jnp.bfloat16)
    upward = jnp.dot(hidden, up_weight, preferred_element_type=jnp.float32)
    active = jnp.square(jax.nn.relu(upward)).astype(jnp.bfloat16)
    downward = jnp.dot(active, down_weight, preferred_element_type=jnp.float32)
    return layer_norm(ALPHA * hidden.astype(jnp.float32) + downward, final_gain).astype(jnp.bfloat16)
```

```python
import functools

import jax
import jax.numpy as jnp
from jax import lax
from jax.sharding import Mesh
from jax.sharding import PartitionSpec as P

HDIM = 64
BLK = 128
KV = ("y", "xh", "xl")
KV_ROWS = ("xl", "y", "xh")
TP = ("z", "c")

ALPHA = 2.0**0.5
EPS = 1e-05
F32 = jnp.float32
BF16 = jnp.bfloat16


def copy_for_each(x, axis):
    peers = lax.axis_size(axis)
    return lax.all_to_all(jnp.broadcast_to(x[None], (peers, *x.shape)), axis, 0, 0, tiled=True)


def gather_tp(x):
    parts = copy_for_each(x, "z")
    both = lax.all_gather(parts, "c", tiled=False)
    return both.reshape(-1, x.shape[1])


def scatter_tp(x):
    n = x.shape[1]
    halves = x.reshape(2, -1, n)
    core = lax.axis_index("c")
    mine = lax.dynamic_index_in_dim(halves, core, 0, keepdims=False)
    other = lax.dynamic_index_in_dim(halves, 1 - core, 0, keepdims=False).astype(BF16)
    arrived = lax.ppermute(other, "c", [(0, 1), (1, 0)])
    pair = (mine + arrived.astype(F32)).astype(BF16)
    parts = lax.all_to_all(pair.reshape(8, -1, n), "z", 0, 0, tiled=True)
    return parts.astype(F32).sum(axis=0)


def scatter_kv(x):
    n = x.shape[1]
    arrived = lax.all_to_all(x.astype(BF16).reshape(16, -1, n), KV_ROWS, 0, 0, tiled=True)
    return arrived.astype(F32).sum(axis=0)


def gather_kv(x):
    return copy_for_each(x, KV_ROWS).reshape(-1, x.shape[1])


def rotate(vectors, positions):
    half = vectors.shape[-1] // 2
    inverse = 10000.0 ** (-jnp.arange(half, dtype=jnp.float32) / half)
    angle = positions.astype(jnp.float32)[:, None] * inverse[None, :]
    cosine = jnp.cos(angle)[:, None, :]
    sine = jnp.sin(angle)[:, None, :]
    former, latter = (vectors[..., :half], vectors[..., half:])
    return jnp.concatenate([former * cosine - latter * sine, latter * cosine + former * sine], -1)


def normalize(values, gain):
    width = values.shape[1] * lax.axis_size(KV)
    sums = jnp.stack([jnp.sum(values, 1), jnp.sum(values * values, 1)])
    total, square = lax.psum(lax.psum(sums, "y"), ("xh", "xl"))
    mean = total / width
    centred = values - mean[:, None]
    spread = square / width - mean * mean
    return centred * lax.rsqrt(spread[:, None] + EPS) * gain[None, :]


def retain(query, keyed, valued, gated, lengths, state, keys, values, rate, gain):
    count = query.shape[0]
    heads = rate.shape[0]
    q_rot = rotate(query.astype(jnp.float32).reshape(count, heads, HDIM), lengths).astype(
        jnp.bfloat16
    )
    k_rot = (rotate(keyed.astype(jnp.float32).reshape(count, heads, HDIM), lengths) * 0.125).astype(
        jnp.bfloat16
    )
    v_new = valued.astype(jnp.float32).reshape(count, heads, HDIM)
    cached_k = keys.reshape(count, BLK, heads, HDIM)
    cached_v = values.reshape(count, BLK, heads, HDIM)
    scores = jnp.einsum("shn,sihn->shi", q_rot, cached_k, preferred_element_type=jnp.float32)
    offset = lengths % BLK
    slots = jnp.arange(BLK, dtype=jnp.int32)
    lag = jnp.maximum(offset[:, None] - slots[None, :], 0).astype(jnp.float32)
    live = (slots[None, :] < offset[:, None])[:, None, :]
    factor = jnp.where(live, jnp.exp(-rate[None, :, None] * lag[:, None, :]), 0.0)
    weights = (scores * factor).astype(jnp.bfloat16)
    own = jnp.einsum("shn,shn->sh", q_rot, k_rot, preferred_element_type=jnp.float32).astype(
        jnp.bfloat16
    )
    inner = jnp.einsum("shi,sihn->shn", weights, cached_v, preferred_element_type=jnp.float32)
    inner = inner + own.astype(jnp.float32)[..., None] * v_new
    carried = jnp.exp(-rate[None, :] * (offset[:, None] + 1).astype(jnp.float32))
    cross = (
        jnp.einsum(
            "shk,skhv->shv", q_rot.astype(jnp.float32), state.reshape(count, HDIM, heads, HDIM)
        )
        * carried[..., None]
    )
    retained = inner + cross
    mean = jnp.mean(retained, -1, keepdims=True)
    centred = retained - mean
    spread = jnp.mean(centred * centred, -1, keepdims=True)
    normed = centred * lax.rsqrt(spread + EPS) * gain.reshape(heads, HDIM)[None]
    gate_f = jax.nn.silu(gated.astype(jnp.float32).reshape(count, heads, HDIM))
    return (gate_f * normed).reshape(count, heads * HDIM).astype(jnp.bfloat16)


def per_device(
    tokens,
    lengths,
    state_block,
    cached_keys,
    cached_values,
    query_weight,
    key_weight,
    value_weight,
    gate_weight,
    decay_rate,
    head_gain,
    out_weight,
    mixer_gain,
    up_weight,
    down_weight,
    final_gain,
):
    width = query_weight.shape[1]
    joined = jnp.concatenate([query_weight, key_weight, value_weight, gate_weight], 1)
    all_rows = gather_tp(tokens)
    summed = scatter_kv(jnp.dot(all_rows, joined, preferred_element_type=F32)).astype(BF16)
    query, keyed, valued, gated = [
        summed[:, index * width : (index + 1) * width] for index in range(4)
    ]
    mixed = retain(
        query,
        keyed,
        valued,
        gated,
        lengths,
        state_block,
        cached_keys,
        cached_values,
        decay_rate,
        head_gain,
    )
    branch = scatter_tp(jnp.dot(gather_kv(mixed), out_weight, preferred_element_type=F32))
    hidden = normalize(ALPHA * tokens.astype(F32) + branch, mixer_gain).astype(BF16)
    upward = scatter_kv(jnp.dot(gather_tp(hidden), up_weight, preferred_element_type=F32))
    active = jnp.square(jax.nn.relu(upward)).astype(BF16)
    downward = scatter_tp(jnp.dot(gather_kv(active), down_weight, preferred_element_type=F32))
    result = normalize(ALPHA * hidden.astype(F32) + downward, final_gain)
    return result.astype(BF16)


def solution(mesh):
    finer = Mesh(mesh.devices.reshape(4, 2, 2, 8, 2), ("y", "xh", "xl", "z", "c"))
    placed = (
        P(TP, KV),
        P(KV),
        P(KV, None, TP),
        P(KV, None, TP),
        P(KV, None, TP),
        P(KV, TP),
        P(KV, TP),
        P(KV, TP),
        P(KV, TP),
        P(TP),
        P(TP),
        P(TP, KV),
        P(KV),
        P(KV, TP),
        P(TP, KV),
        P(KV),
    )
    return jax.shard_map(
        per_device, mesh=finer, in_specs=placed, out_specs=P(TP, KV), check_vma=False
    )
```

```python
import functools

import jax
import jax.numpy as jnp
from jax import lax
from jax.sharding import Mesh
from jax.sharding import PartitionSpec as P

HDIM = 64
BLK = 128
KV = ("y", "xh", "xl")
KV_ROWS = ("xl", "y", "xh")
TP = ("z", "c")
X = ("xh", "xl")

ALPHA = 2.0**0.5
EPS = 1e-05
F32 = jnp.float32
BF16 = jnp.bfloat16


def copy_for_each(x, axis):
    peers = lax.axis_size(axis)
    return lax.all_to_all(jnp.broadcast_to(x[None], (peers, *x.shape)), axis, 0, 0, tiled=True)


def gather_tp(x):
    parts = copy_for_each(x, "z")
    both = lax.all_gather(parts, "c", tiled=False)
    return both.reshape(-1, x.shape[1])


def scatter_tp(x):
    n = x.shape[1]
    halves = x.reshape(2, -1, n)
    core = lax.axis_index("c")
    mine = lax.dynamic_index_in_dim(halves, core, 0, keepdims=False)
    other = lax.dynamic_index_in_dim(halves, 1 - core, 0, keepdims=False).astype(BF16)
    arrived = lax.ppermute(other, "c", [(0, 1), (1, 0)])
    pair = (mine + arrived.astype(F32)).astype(BF16)
    parts = lax.all_to_all(pair.reshape(8, -1, n), "z", 0, 0, tiled=True)
    return parts.astype(F32).sum(axis=0)


def scatter_kv(x):
    n = x.shape[1]
    arrived = lax.all_to_all(x.astype(BF16).reshape(16, -1, n), KV_ROWS, 0, 0, tiled=True)
    return arrived.astype(F32).sum(axis=0)


def rotate(vectors, positions):
    half = vectors.shape[-1] // 2
    inverse = 10000.0 ** (-jnp.arange(half, dtype=jnp.float32) / half)
    angle = positions.astype(jnp.float32)[:, None] * inverse[None, :]
    cosine = jnp.cos(angle)[:, None, :]
    sine = jnp.sin(angle)[:, None, :]
    former, latter = (vectors[..., :half], vectors[..., half:])
    return jnp.concatenate([former * cosine - latter * sine, latter * cosine + former * sine], -1)


def apart(x):
    high = lax.reduce_precision(x, 8, 7)
    rest = x - high
    middle = lax.reduce_precision(rest, 8, 7)
    return high.astype(BF16), middle.astype(BF16), (rest - middle).astype(BF16)


def rolled(x, start):
    return lax.dynamic_slice_in_dim(jnp.concatenate([x, x]), start, 4)


def to_peers(x):
    rest = x.shape[1:]
    x = x.reshape(2, 2, *rest).swapaxes(0, 1)
    return jnp.broadcast_to(x[:, None], (2, 4, 2, *rest)).reshape(16, *rest)


def own_y(x):
    rest = x.shape[1:]
    x = x.reshape(2, 4, 2, *rest)
    x = lax.dynamic_index_in_dim(x, lax.axis_index("y"), 1, keepdims=False)
    return x.swapaxes(0, 1).reshape(4, *rest)


def gather_weights(out_weight, up_weight, down_weight, gain):
    forward = [(i, (i + 1) % 4) for i in range(4)]
    back = [(i, (i + 3) % 4) for i in range(4)]
    up_rows = up_weight.reshape(256, 4, 256).swapaxes(0, 1).reshape(1024, 256)
    gains = jnp.stack(apart(gain) + (jnp.zeros((256,), BF16),) * 5)
    packed = jnp.concatenate([up_rows, out_weight, down_weight, gains])
    cut = 1152
    before = lax.ppermute(packed, X, forward)
    after = lax.ppermute(packed, X, back)
    first = lax.ppermute(before[:cut], X, forward)
    second = lax.ppermute(after[cut:], X, back)
    firsts = [packed[:cut], after[:cut], first, before[:cut]]
    seconds = [packed[cut:], after[cut:], second, before[cut:]]
    up = jnp.concatenate(
        [p[:1024].reshape(4, 256, 256).swapaxes(0, 1).reshape(256, 1024) for p in firsts]
    )
    out = jnp.concatenate([p[1024:] for p in firsts], 1)
    down = jnp.concatenate([p[:1024] for p in seconds], 1)
    gain = jnp.concatenate([p[1024:1027].astype(F32).sum(0) for p in seconds])
    return out, up, down, gain


def retain(query, keyed, valued, gated, lengths, state, keys, values, rate, gain):
    count = query.shape[0]
    heads = rate.shape[0]
    q_rot = rotate(query.astype(jnp.float32).reshape(count, heads, HDIM), lengths).astype(
        jnp.bfloat16
    )
    k_rot = (rotate(keyed.astype(jnp.float32).reshape(count, heads, HDIM), lengths) * 0.125).astype(
        jnp.bfloat16
    )
    v_new = valued.astype(jnp.float32).reshape(count, heads, HDIM)
    cached_k = keys.reshape(count, BLK, heads, HDIM)
    cached_v = values.reshape(count, BLK, heads, HDIM)
    scores = jnp.einsum("shn,sihn->shi", q_rot, cached_k, preferred_element_type=jnp.float32)
    offset = lengths % BLK
    slots = jnp.arange(BLK, dtype=jnp.int32)
    lag = jnp.maximum(offset[:, None] - slots[None, :], 0).astype(jnp.float32)
    live = (slots[None, :] < offset[:, None])[:, None, :]
    factor = jnp.where(live, jnp.exp(-rate[None, :, None] * lag[:, None, :]), 0.0)
    weights = (scores * factor).astype(jnp.bfloat16)
    own = jnp.einsum("shn,shn->sh", q_rot, k_rot, preferred_element_type=jnp.float32).astype(
        jnp.bfloat16
    )
    inner = jnp.einsum("shi,sihn->shn", weights, cached_v, preferred_element_type=jnp.float32)
    inner = inner + own.astype(jnp.float32)[..., None] * v_new
    carried = jnp.exp(-rate[None, :] * (offset[:, None] + 1).astype(jnp.float32))
    cross = (
        jnp.einsum(
            "shk,skhv->shv", q_rot.astype(jnp.float32), state.reshape(count, HDIM, heads, HDIM)
        )
        * carried[..., None]
    )
    retained = inner + cross
    mean = jnp.mean(retained, -1, keepdims=True)
    centred = retained - mean
    spread = jnp.mean(centred * centred, -1, keepdims=True)
    normed = centred * lax.rsqrt(spread + EPS) * gain.reshape(heads, HDIM)[None]
    gate_f = jax.nn.silu(gated.astype(jnp.float32).reshape(count, heads, HDIM))
    return (gate_f * normed).reshape(count, heads * HDIM).astype(jnp.bfloat16)


def per_device(
    tokens,
    lengths,
    state_block,
    cached_keys,
    cached_values,
    query_weight,
    key_weight,
    value_weight,
    gate_weight,
    decay_rate,
    head_gain,
    out_weight,
    mixer_gain,
    up_weight,
    down_weight,
    final_gain,
):
    width = query_weight.shape[1]
    joined = jnp.concatenate([query_weight, key_weight, value_weight, gate_weight], 1)
    all_rows = gather_tp(tokens)
    summed = scatter_kv(jnp.dot(all_rows, joined, preferred_element_type=F32)).astype(BF16)
    query, keyed, valued, gated = [
        summed[:, index * width : (index + 1) * width] for index in range(4)
    ]
    mixed = retain(
        query,
        keyed,
        valued,
        gated,
        lengths,
        state_block,
        cached_keys,
        cached_values,
        decay_rate,
        head_gain,
    )
    out_rel, up_rel, down_rel, gain_rel = gather_weights(
        out_weight, up_weight, down_weight, mixer_gain
    )
    place = lax.axis_index(X)

    sent = jnp.concatenate([mixed.reshape(4, 16, 128), tokens.reshape(4, 16, 256)], 2)
    came = lax.all_to_all(to_peers(sent), KV_ROWS, 0, 0, tiled=True)
    mixed_rows = came[:, :, :128].reshape(256, 128)
    token_rows = rolled(own_y(came[:, :, 128:]), place).swapaxes(0, 1).reshape(16, 1024)

    branch = scatter_tp(jnp.dot(mixed_rows, out_rel, preferred_element_type=F32))
    values = ALPHA * token_rows.astype(F32) + branch
    gained = (values * gain_rel[None]).astype(BF16)
    all_gained = gather_tp(gained)

    plain = all_gained.astype(F32) / gain_rel[None]
    sums = jnp.stack([plain.sum(1).reshape(4, 64), (plain * plain).sum(1).reshape(4, 64)], 1)
    sum_parts = jnp.stack(apart(sums), 1).reshape(4, 1, 384)
    gain_row = jnp.dot(jnp.stack(apart(gain_rel)), up_rel, preferred_element_type=F32)
    gain_row = gain_row.sum(0, keepdims=True).astype(BF16)
    extra = jnp.concatenate(
        [
            jnp.broadcast_to(gain_row[None], (4, 1, 1024)),
            jnp.pad(sum_parts, ((0, 0), (0, 0), (0, 640))),
            jnp.zeros((4, 6, 1024), BF16),
        ],
        1,
    )
    product = jnp.dot(all_gained, up_rel, preferred_element_type=F32).astype(BF16)
    came = lax.all_to_all(
        jnp.concatenate([product.reshape(4, 64, 1024), extra], 1), "y", 0, 0, tiled=True
    )
    total = came.astype(F32).sum(0)
    sums = total[65, :384].reshape(3, 2, 64).sum(0)
    mean = sums[0] / 4096
    inverse = lax.rsqrt(sums[1] / 4096 - mean * mean + EPS)
    upward = (total[:64] - mean[:, None] * total[64:65]) * inverse[:, None]
    active = jnp.square(jax.nn.relu(upward)).astype(BF16)
    stat_parts = jnp.stack(apart(jnp.stack([mean, inverse]))).reshape(1, 384)
    block = jnp.concatenate(
        [active, jnp.pad(stat_parts, ((0, 7), (0, 640)))]
    )
    came = copy_for_each(block, "y")
    downward = scatter_tp(
        jnp.dot(came[:, :64].reshape(256, 1024), down_rel, preferred_element_type=F32)
    )
    stats = came[:, 64, :384].astype(F32).reshape(4, 3, 2, 64).sum(1)
    stats = stats.swapaxes(0, 1).reshape(2, 16, 16)
    index = lax.axis_index("c") * 8 + lax.axis_index("z")
    mean, inverse = lax.dynamic_index_in_dim(stats, index, 1, keepdims=False)
    hidden = (gained.astype(F32) - mean[:, None] * gain_rel[None]) * inverse[:, None]
    last = ALPHA * hidden + downward

    sums = jnp.stack([last.sum(1), (last * last).sum(1)], 1)
    sum_parts = jnp.concatenate(apart(sums), 1)
    pieces = rolled(last.astype(BF16).reshape(16, 4, 256).swapaxes(0, 1), (4 - place) % 4)
    sums_sent = jnp.broadcast_to(jnp.pad(sum_parts, ((0, 0), (0, 122)))[None], (4, 16, 128))
    came = lax.all_to_all(
        to_peers(jnp.concatenate([pieces, sums_sent], 2)), KV_ROWS, 0, 0, tiled=True
    )
    last = own_y(came[:, :, :256]).reshape(64, 256).astype(F32)
    sums = came[:, :, 256:262].astype(F32).reshape(2, 4, 2, 16, 3, 2).sum((1, 4))
    sums = sums.swapaxes(0, 1).reshape(64, 2)
    mean = sums[:, 0] / 4096
    inverse = lax.rsqrt(sums[:, 1] / 4096 - mean * mean + EPS)
    return ((last - mean[:, None]) * inverse[:, None] * final_gain[None]).astype(BF16)


def solution(mesh):
    finer = Mesh(mesh.devices.reshape(4, 2, 2, 8, 2), ("y", "xh", "xl", "z", "c"))
    placed = (
        P(TP, KV),
        P(KV),
        P(KV, None, TP),
        P(KV, None, TP),
        P(KV, None, TP),
        P(KV, TP),
        P(KV, TP),
        P(KV, TP),
        P(KV, TP),
        P(TP),
        P(TP),
        P(TP, KV),
        P(KV),
        P(KV, TP),
        P(TP, KV),
        P(KV),
    )
    return jax.shard_map(
        per_device, mesh=finer, in_specs=placed, out_specs=P(TP, KV), check_vma=False
    )
```

```python
import jax
import jax.numpy as jnp
from jax import lax
from jax.experimental import pallas as pl
from jax.experimental.pallas import tpu as pltpu
from jax.sharding import Mesh
from jax.sharding import PartitionSpec as P

HDIM = 64
BLK = 128
KV = ("y", "xh", "xl")
KV_ROWS = ("xl", "y", "xh")
TP = ("z", "c")
X = ("xh", "xl")

ALPHA = 2.0**0.5
EPS = 1e-05
F32 = jnp.float32
BF16 = jnp.bfloat16


def copy_for_each(x, axis):
    peers = lax.axis_size(axis)
    return lax.all_to_all(jnp.broadcast_to(x[None], (peers, *x.shape)), axis, 0, 0, tiled=True)


def gather_tp(x):
    parts = copy_for_each(x, "z")
    both = lax.all_gather(parts, "c", tiled=False)
    return both.reshape(-1, x.shape[1])


def scatter_tp(x):
    n = x.shape[1]
    halves = x.reshape(2, -1, n)
    core = lax.axis_index("c")
    mine = lax.dynamic_index_in_dim(halves, core, 0, keepdims=False)
    other = lax.dynamic_index_in_dim(halves, 1 - core, 0, keepdims=False).astype(BF16)
    arrived = lax.ppermute(other, "c", [(0, 1), (1, 0)])
    pair = (mine + arrived.astype(F32)).astype(BF16)
    parts = lax.all_to_all(pair.reshape(8, -1, n), "z", 0, 0, tiled=True)
    return parts.astype(F32).sum(axis=0)


def apart(x):
    high = lax.reduce_precision(x, 8, 7)
    rest = x - high
    middle = lax.reduce_precision(rest, 8, 7)
    return high.astype(BF16), middle.astype(BF16), (rest - middle).astype(BF16)


def rolled(x, start):
    return lax.dynamic_slice_in_dim(jnp.concatenate([x, x]), start, 4)


def to_peers(x):
    rest = x.shape[1:]
    x = x.reshape(2, 2, *rest).swapaxes(0, 1)
    return jnp.broadcast_to(x[:, None], (2, 4, 2, *rest)).reshape(16, *rest)


def own_y(x):
    rest = x.shape[1:]
    x = x.reshape(2, 4, 2, *rest)
    x = lax.dynamic_index_in_dim(x, lax.axis_index("y"), 1, keepdims=False)
    return x.swapaxes(0, 1).reshape(4, *rest)


def copied(kernel, out_shape, copies, *args):
    many = isinstance(out_shape, tuple)
    vmem = pl.BlockSpec(memory_space=pltpu.VMEM)
    return pl.pallas_call(
        kernel,
        out_shape=out_shape,
        in_specs=[pl.BlockSpec(memory_space=pl.ANY)] * len(args),
        out_specs=(vmem,) * len(out_shape) if many else vmem,
        scratch_shapes=[pltpu.SemaphoreType.DMA((copies,))],
    )(*args)


def run_copies(pairs, sems):
    started = [
        pltpu.make_async_copy(source, target, sems.at[i]) for i, (source, target) in enumerate(pairs)
    ]
    for one in started:
        one.start()
    for one in started:
        one.wait()


def stack_kernel(own, after, far, before, stacked, sems):
    parts = (own, after, far, before)
    run_copies([(p, stacked.at[pl.ds(256 * i, 256)]) for i, p in enumerate(parts)], sems)


def beside_kernel(own, after, far, before, joined, sems):
    parts = (own, after, far, before)
    run_copies([(p, joined.at[:, pl.ds(256 * i, 256)]) for i, p in enumerate(parts)], sems)


def out_kernel(own, after, far, before, joined, gain):
    for i, p in enumerate((own, after, far, before)):
        lanes = pl.ds(256 * i, 256)
        joined[:, lanes] = p[:128]
        gain[:, lanes] = p[128:131].astype(F32).sum(0, keepdims=True)


def x_slots(x):
    forward = [(i, (i + 1) % 4) for i in range(4)]
    back = [(i, (i + 3) % 4) for i in range(4)]
    before = lax.ppermute(x, X, forward)
    after = lax.ppermute(x, X, back)
    far = lax.ppermute(before, X, forward)
    return x, after, far, before


def head_sum(x):
    sums = [x[:, :HDIM].sum(1, keepdims=True), x[:, HDIM:].sum(1, keepdims=True)]
    return jnp.where(lax.broadcasted_iota(jnp.int32, x.shape, 1) < HDIM, *sums)


def retain_kernel(
    came, cosine, sine, offset, rate, gain, swap, ones, tokens, keys, values, state, sent
):
    summed = came[...].astype(F32).sum(0).astype(BF16)
    query, keyed, valued, gated = [summed[:, 128 * i : 128 * i + 128] for i in range(4)]

    def rotated(u):
        swapped = jnp.dot(u, swap[...], preferred_element_type=F32)
        return u.astype(F32) * cosine[...] + swapped * sine[...]

    q_rot = rotated(query).astype(BF16).astype(F32)
    k_rot = (rotated(keyed) * 0.125).astype(BF16).astype(F32)
    own = head_sum(q_rot * k_rot).astype(BF16).astype(F32)
    slot = lax.broadcasted_iota(jnp.int32, (BLK, 128), 0).astype(F32)
    growth = jnp.exp(rate[...] * slot)
    key_index = lax.broadcasted_iota(jnp.int32, (HDIM, 128), 0)
    same = key_index == lax.broadcasted_iota(jnp.int32, (HDIM, 128), 1) % HDIM
    inner, cross = [], []
    for s in range(16):
        row = q_rot[s : s + 1]
        terms = jnp.concatenate(
            [(keys[s].astype(F32) * row).astype(BF16), jnp.where(same, row, 0.0).astype(BF16)]
        )
        spread = jnp.dot(terms, ones[...], preferred_element_type=F32)
        weights = jnp.where(slot < offset[s : s + 1], spread[:BLK] * growth, 0.0)
        inner.append((weights * values[s].astype(F32)).sum(0, keepdims=True))
        cross.append((spread[BLK:] * state[s]).sum(0, keepdims=True))
    inner = jnp.concatenate(inner) * jnp.exp(-rate[...] * offset[...])
    cross = jnp.concatenate(cross) * jnp.exp(-rate[...] * (offset[...] + 1.0))
    retained = inner + own * valued.astype(F32) + cross
    centred = retained - head_sum(retained) / HDIM
    variance = head_sum(centred * centred) / HDIM
    normed = centred * lax.rsqrt(variance + EPS) * gain[...]
    mixed = (jax.nn.silu(gated.astype(F32)) * normed).astype(BF16)
    for y in range(4):
        sent[0, y, 0, :, :128] = mixed
        sent[0, y, 0, :, 128:] = tokens[...]


def retain(came, lengths, state, keys, values, rate, gain, tokens):
    lane = jnp.arange(128)
    inverse = 10000.0 ** (-(lane % 32).astype(F32) / 32)
    angle = lengths.astype(F32)[:, None] * inverse[None]
    sine = jnp.sin(angle) * jnp.where(lane % HDIM < 32, -1.0, 1.0)[None]
    swap = (lane[:, None] == (lane ^ 32)[None]).astype(BF16)
    ones = (lane[:, None] // HDIM == lane[None] // HDIM).astype(BF16)
    offset = jnp.broadcast_to((lengths % BLK).astype(F32)[:, None], (64, 128))

    def rows(*rest):
        return pl.BlockSpec((16, *rest), lambda i: (i,) + (0,) * len(rest))

    def whole(*shape):
        return pl.BlockSpec(shape, lambda i: (0,) * len(shape))

    sent = pl.pallas_call(
        retain_kernel,
        grid=(4,),
        out_shape=jax.ShapeDtypeStruct((2, 4, 2, 16, 384), BF16),
        in_specs=[
            pl.BlockSpec((16, 16, 512), lambda i: (0, i, 0)),
            rows(128),
            rows(128),
            rows(128),
            whole(1, 128),
            whole(1, 128),
            whole(128, 128),
            whole(128, 128),
            rows(256),
            rows(BLK, 128),
            rows(BLK, 128),
            rows(HDIM, 128),
        ],
        out_specs=pl.BlockSpec((1, 4, 1, 16, 384), lambda i: (i % 2, 0, i // 2, 0, 0)),
    )(
        came,
        jnp.cos(angle),
        sine,
        offset,
        jnp.repeat(rate, HDIM)[None],
        gain[None],
        swap,
        ones,
        tokens,
        keys,
        values,
        state,
    )
    return sent.reshape(16, 16, 384)


def per_device(
    tokens,
    lengths,
    state_block,
    cached_keys,
    cached_values,
    query_weight,
    key_weight,
    value_weight,
    gate_weight,
    decay_rate,
    head_gain,
    out_weight,
    mixer_gain,
    up_weight,
    down_weight,
    final_gain,
):
    joined = jnp.concatenate([query_weight, key_weight, value_weight, gate_weight], 1)
    all_rows = gather_tp(tokens)
    partial = jnp.dot(all_rows, joined, preferred_element_type=F32).astype(BF16)
    came = lax.all_to_all(partial.reshape(16, 64, 512), KV_ROWS, 0, 0, tiled=True)
    sent = retain(
        came,
        lengths,
        state_block,
        cached_keys,
        cached_values,
        decay_rate,
        head_gain,
        tokens,
    )
    packed = jnp.concatenate(
        [out_weight, jnp.stack(apart(mixer_gain) + (jnp.zeros((256,), BF16),) * 5)]
    )
    out_slots = x_slots(packed)
    out_rel, gain_rel = pl.pallas_call(
        out_kernel,
        out_shape=(jax.ShapeDtypeStruct((128, 1024), BF16), jax.ShapeDtypeStruct((1, 1024), F32)),
    )(*out_slots)
    gain_rel = gain_rel[0]
    square = jax.ShapeDtypeStruct((1024, 1024), BF16)
    up_slots = x_slots(up_weight)
    up_rel = copied(stack_kernel, square, 4, *up_slots)
    down_slots = x_slots(down_weight)
    down_rel = copied(beside_kernel, square, 4, *down_slots)
    place = lax.axis_index(X)

    came = lax.all_to_all(sent, KV_ROWS, 0, 0, tiled=True)
    mixed_rows = came[:, :, :128].reshape(256, 128)
    token_rows = rolled(own_y(came[:, :, 128:]), place).swapaxes(0, 1).reshape(16, 1024)

    partial = jnp.dot(mixed_rows, out_rel, preferred_element_type=F32)
    branch = scatter_tp(partial)
    values = ALPHA * token_rows.astype(F32) + branch
    gained = (values * gain_rel[None]).astype(BF16)
    all_gained = gather_tp(gained)

    plain = all_gained.astype(F32) / gain_rel[None]
    sums = jnp.stack([plain.sum(1).reshape(4, 64), (plain * plain).sum(1).reshape(4, 64)], 1)
    sum_parts = jnp.stack(apart(sums), 1).reshape(4, 1, 384)
    gain_row = jnp.dot(jnp.stack(apart(gain_rel)), up_rel, preferred_element_type=F32)
    gain_row = gain_row.sum(0, keepdims=True).astype(BF16)
    extra = jnp.concatenate(
        [
            jnp.broadcast_to(gain_row[None], (4, 1, 1024)),
            jnp.pad(sum_parts, ((0, 0), (0, 0), (0, 640))),
            jnp.zeros((4, 6, 1024), BF16),
        ],
        1,
    )
    product = jnp.dot(all_gained, up_rel, preferred_element_type=F32).astype(BF16)
    sent = jnp.concatenate([product.reshape(4, 64, 1024), extra], 1)
    came = lax.all_to_all(sent, "y", 0, 0, tiled=True)
    total = came.astype(F32).sum(0)
    sums = total[65, :384].reshape(3, 2, 64).sum(0)
    mean = sums[0] / 4096
    inverse = lax.rsqrt(sums[1] / 4096 - mean * mean + EPS)
    upward = (total[:64] - mean[:, None] * total[64:65]) * inverse[:, None]
    active = jnp.square(jax.nn.relu(upward)).astype(BF16)
    stat_parts = jnp.stack(apart(jnp.stack([mean, inverse]))).reshape(1, 384)
    block = jnp.concatenate(
        [active, jnp.pad(stat_parts, ((0, 7), (0, 640)))]
    )
    came = copy_for_each(block, "y")
    downward = scatter_tp(
        jnp.dot(came[:, :64].reshape(256, 1024), down_rel, preferred_element_type=F32)
    )
    stats = came[:, 64, :384].astype(F32).reshape(4, 3, 2, 64).sum(1)
    stats = stats.swapaxes(0, 1).reshape(2, 16, 16)
    index = lax.axis_index("c") * 8 + lax.axis_index("z")
    mean, inverse = lax.dynamic_index_in_dim(stats, index, 1, keepdims=False)
    hidden = (gained.astype(F32) - mean[:, None] * gain_rel[None]) * inverse[:, None]
    last = ALPHA * hidden + downward

    sums = jnp.stack([last.sum(1), (last * last).sum(1)], 1)
    sum_parts = jnp.concatenate(apart(sums), 1)
    pieces = rolled(last.astype(BF16).reshape(16, 4, 256).swapaxes(0, 1), (4 - place) % 4)
    sums_sent = jnp.broadcast_to(jnp.pad(sum_parts, ((0, 0), (0, 122)))[None], (4, 16, 128))
    came = lax.all_to_all(
        to_peers(jnp.concatenate([pieces, sums_sent], 2)), KV_ROWS, 0, 0, tiled=True
    )
    last = own_y(came[:, :, :256]).reshape(64, 256).astype(F32)
    sums = came[:, :, 256:262].astype(F32).reshape(2, 4, 2, 16, 3, 2).sum((1, 4))
    sums = sums.swapaxes(0, 1).reshape(64, 2)
    mean = sums[:, 0] / 4096
    inverse = lax.rsqrt(sums[:, 1] / 4096 - mean * mean + EPS)
    return ((last - mean[:, None]) * inverse[:, None] * final_gain[None]).astype(BF16)


def solution(mesh):
    finer = Mesh(mesh.devices.reshape(4, 2, 2, 8, 2), ("y", "xh", "xl", "z", "c"))
    placed = (
        P(TP, KV),
        P(KV),
        P(KV, None, TP),
        P(KV, None, TP),
        P(KV, None, TP),
        P(KV, TP),
        P(KV, TP),
        P(KV, TP),
        P(KV, TP),
        P(TP),
        P(TP),
        P(TP, KV),
        P(KV),
        P(KV, TP),
        P(TP, KV),
        P(KV),
    )

    return jax.shard_map(per_device, mesh=finer, in_specs=placed, out_specs=P(TP, KV), check_vma=False)
```

```python
import jax
import jax.numpy as jnp
from jax import lax
from jax.experimental import pallas as pl
from jax.experimental.pallas import tpu as pltpu
from jax.sharding import Mesh
from jax.sharding import PartitionSpec as P

HDIM = 64
BLK = 128
KV = ("y", "xh", "xl")
KV_ROWS = ("xl", "y", "xh")
TP = ("z", "c")
X = ("xh", "xl")

ALPHA = 2.0**0.5
EPS = 1e-05
F32 = jnp.float32
BF16 = jnp.bfloat16


def copy_for_each(x, axis):
    peers = lax.axis_size(axis)
    return lax.all_to_all(jnp.broadcast_to(x[None], (peers, *x.shape)), axis, 0, 0, tiled=True)


def gather_tp(x):
    parts = copy_for_each(x, "z")
    both = lax.all_gather(parts, "c", tiled=False)
    return both.reshape(-1, x.shape[1])


def scatter_tp(x):
    n = x.shape[1]
    halves = x.reshape(2, -1, n)
    core = lax.axis_index("c")
    mine = lax.dynamic_index_in_dim(halves, core, 0, keepdims=False)
    other = lax.dynamic_index_in_dim(halves, 1 - core, 0, keepdims=False).astype(BF16)
    arrived = lax.ppermute(other, "c", [(0, 1), (1, 0)])
    pair = (mine + arrived.astype(F32)).astype(BF16)
    parts = lax.all_to_all(pair.reshape(8, -1, n), "z", 0, 0, tiled=True)
    return parts.astype(F32).sum(axis=0)


def apart(x):
    high = lax.reduce_precision(x, 8, 7)
    rest = x - high
    middle = lax.reduce_precision(rest, 8, 7)
    return high.astype(BF16), middle.astype(BF16), (rest - middle).astype(BF16)


def rolled(x, start):
    return lax.dynamic_slice_in_dim(jnp.concatenate([x, x]), start, 4)


def to_peers(x):
    rest = x.shape[1:]
    x = x.reshape(2, 2, *rest).swapaxes(0, 1)
    return jnp.broadcast_to(x[:, None], (2, 4, 2, *rest)).reshape(16, *rest)


def own_y(x):
    rest = x.shape[1:]
    x = x.reshape(2, 4, 2, *rest)
    x = lax.dynamic_index_in_dim(x, lax.axis_index("y"), 1, keepdims=False)
    return x.swapaxes(0, 1).reshape(4, *rest)


def copied(kernel, out_shape, copies, limit, *args):
    many = isinstance(out_shape, tuple)
    vmem = pl.BlockSpec(memory_space=pltpu.VMEM)
    return pl.pallas_call(
        kernel,
        out_shape=out_shape,
        in_specs=[pl.BlockSpec(memory_space=pl.ANY)] * len(args),
        out_specs=(vmem,) * len(out_shape) if many else vmem,
        scratch_shapes=[pltpu.SemaphoreType.DMA((copies,))],
        compiler_params=pltpu.CompilerParams(vmem_limit_bytes=limit),
    )(*args)


def run_copies(pairs, sems):
    started = [
        pltpu.make_async_copy(source, target, sems.at[i]) for i, (source, target) in enumerate(pairs)
    ]
    for one in started:
        one.start()
    for one in started:
        one.wait()


def stack_kernel(own, after, far, before, stacked, sems):
    parts = (own, after, far, before)
    run_copies([(p, stacked.at[pl.ds(256 * i, 256)]) for i, p in enumerate(parts)], sems)


def beside_kernel(own, after, far, before, joined, sems):
    parts = (own, after, far, before)
    run_copies([(p, joined.at[:, pl.ds(256 * i, 256)]) for i, p in enumerate(parts)], sems)


def out_kernel(own, after, far, before, joined, gain):
    for i, p in enumerate((own, after, far, before)):
        lanes = pl.ds(256 * i, 256)
        joined[:, lanes] = p[:128]
        gain[:, lanes] = p[128:131].astype(F32).sum(0, keepdims=True)


def x_slots(x, far_back=False):
    forward = [(i, (i + 1) % 4) for i in range(4)]
    back = [(i, (i + 3) % 4) for i in range(4)]
    before = lax.ppermute(x, X, forward)
    after = lax.ppermute(x, X, back)
    far = lax.ppermute(after, X, back) if far_back else lax.ppermute(before, X, forward)
    return x, after, far, before


def head_sum(x):
    sums = [x[:, :HDIM].sum(1, keepdims=True), x[:, HDIM:].sum(1, keepdims=True)]
    return jnp.where(lax.broadcasted_iota(jnp.int32, x.shape, 1) < HDIM, *sums)


def retain_kernel(came, angles, heads, matrices, tokens, keys, values, state, sent):
    cosine, sine, offset = [angles[:, 128 * i : 128 * i + 128] for i in range(3)]
    rate, gain = heads[0:1], heads[1:2]
    swap, ones = matrices[:128], matrices[128:]

    summed = came[...].astype(F32).sum(0).astype(BF16)
    query, keyed, valued, gated = [summed[:, 128 * i : 128 * i + 128] for i in range(4)]

    def rotated(u):
        swapped = jnp.dot(u, swap, preferred_element_type=F32)
        return u.astype(F32) * cosine + swapped * sine

    q_short = rotated(query).astype(BF16)
    q_rot = q_short.astype(F32)
    k_rot = (rotated(keyed) * 0.125).astype(BF16).astype(F32)
    own = head_sum(q_rot * k_rot).astype(BF16).astype(F32)
    slot = lax.broadcasted_iota(jnp.int32, (BLK, 128), 0).astype(F32)
    growth = jnp.exp(rate * slot)
    key_index = lax.broadcasted_iota(jnp.int32, (HDIM, 128), 0)
    same = key_index == lax.broadcasted_iota(jnp.int32, (HDIM, 128), 1) % HDIM
    same = jnp.where(same, 1.0, 0.0).astype(BF16)
    inner, cross = [], []
    for s in range(64):
        row = q_short[s : s + 1]
        terms = jnp.concatenate([keys[s] * row, same * row])
        spread = jnp.dot(terms, ones, preferred_element_type=F32)
        weights = jnp.where(slot < offset[s : s + 1], spread[:BLK] * growth, 0.0)
        inner.append((weights * values[s].astype(F32)).sum(0, keepdims=True))
        cross.append((spread[BLK:] * state[s]).sum(0, keepdims=True))
    inner = jnp.concatenate(inner) * jnp.exp(-rate * offset)
    cross = jnp.concatenate(cross) * jnp.exp(-rate * (offset + 1.0))
    retained = inner + own * valued.astype(F32) + cross
    centred = retained - head_sum(retained) / HDIM
    variance = head_sum(centred * centred) / HDIM
    normed = centred * lax.rsqrt(variance + EPS) * gain
    mixed = (jax.nn.silu(gated.astype(F32)) * normed).astype(BF16)
    for x in range(4):
        rows = pl.ds(16 * x, 16)
        for y in range(4):
            sent[x % 2, y, x // 2, :, :128] = mixed[16 * x : 16 * x + 16]
            sent[x % 2, y, x // 2, :, 128:] = tokens[rows]


def retain(came, lengths, state, keys, values, rate, gain, tokens):
    lane = jnp.arange(384)
    inverse = 10000.0 ** (-(lane % 32).astype(F32) / 32)
    angle = lengths.astype(F32)[:, None] * inverse[None]
    sine = jnp.sin(angle) * jnp.where(lane % HDIM < 32, -1.0, 1.0)[None]
    offset = (lengths % BLK).astype(F32)[:, None]
    angles = jnp.where(lane < 128, jnp.cos(angle), jnp.where(lane < 256, sine, offset))
    lane = lane[:128]
    swap = (lane[:, None] == (lane ^ 32)[None]).astype(BF16)
    ones = (lane[:, None] // HDIM == lane[None] // HDIM).astype(BF16)
    arrays = (
        came,
        angles,
        jnp.stack([jnp.repeat(rate, HDIM), gain]),
        jnp.concatenate([swap, ones]),
        tokens,
    )
    sent = pl.pallas_call(
        retain_kernel,
        out_shape=jax.ShapeDtypeStruct((2, 4, 2, 16, 384), BF16),
        in_specs=[pl.BlockSpec(memory_space=pltpu.VMEM)] * 8,
        out_specs=pl.BlockSpec(memory_space=pltpu.VMEM),
        compiler_params=pltpu.CompilerParams(vmem_limit_bytes=20 * 2**20),
    )(*arrays, keys, values, state)
    return sent.reshape(16, 16, 384)


def per_device(
    tokens,
    lengths,
    state_block,
    cached_keys,
    cached_values,
    query_weight,
    key_weight,
    value_weight,
    gate_weight,
    decay_rate,
    head_gain,
    out_weight,
    mixer_gain,
    up_weight,
    down_weight,
    final_gain,
):
    joined = lax.optimization_barrier(
        jnp.concatenate([query_weight, key_weight, value_weight, gate_weight], 1)
    )
    all_rows = gather_tp(tokens)
    partial = jnp.dot(all_rows, joined, preferred_element_type=F32).astype(BF16)
    came = lax.all_to_all(partial.reshape(16, 64, 512), KV_ROWS, 0, 0, tiled=True)
    sent = retain(
        came,
        lengths,
        state_block,
        cached_keys,
        cached_values,
        decay_rate,
        head_gain,
        tokens,
    )
    packed = jnp.concatenate(
        [out_weight, jnp.stack(apart(mixer_gain) + (jnp.zeros((256,), BF16),) * 5)]
    )
    out_slots = x_slots(packed)
    out_rel, gain_rel = pl.pallas_call(
        out_kernel,
        out_shape=(jax.ShapeDtypeStruct((128, 1024), BF16), jax.ShapeDtypeStruct((1, 1024), F32)),
        compiler_params=pltpu.CompilerParams(vmem_limit_bytes=4 * 2**20),
    )(*out_slots)
    gain_rel = gain_rel[0]
    square = jax.ShapeDtypeStruct((1024, 1024), BF16)
    up_slots = x_slots(up_weight)
    up_rel = copied(stack_kernel, square, 4, None, *up_slots)
    down_slots = x_slots(down_weight, far_back=True)
    down_rel = copied(beside_kernel, square, 4, None, *down_slots)
    place = lax.axis_index(X)

    came = lax.all_to_all(sent, KV_ROWS, 0, 0, tiled=True)
    mixed_rows = came[:, :, :128].reshape(256, 128)
    token_rows = rolled(own_y(came[:, :, 128:]), place).swapaxes(0, 1).reshape(16, 1024)

    partial = jnp.dot(mixed_rows, out_rel, preferred_element_type=F32)
    branch = scatter_tp(partial)
    values = ALPHA * token_rows.astype(F32) + branch
    gained = (values * gain_rel[None]).astype(BF16)
    all_gained = gather_tp(gained)

    plain = all_gained.astype(F32) / gain_rel[None]
    sums = jnp.stack([plain.sum(1).reshape(4, 64), (plain * plain).sum(1).reshape(4, 64)], 1)
    sum_parts = jnp.stack(apart(sums), 1).reshape(4, 1, 384)
    gain_row = jnp.dot(jnp.stack(apart(gain_rel)), up_rel, preferred_element_type=F32)
    gain_row = gain_row.sum(0, keepdims=True).astype(BF16)
    extra = jnp.concatenate(
        [
            jnp.broadcast_to(gain_row[None], (4, 1, 1024)),
            jnp.pad(sum_parts, ((0, 0), (0, 0), (0, 640))),
            jnp.zeros((4, 6, 1024), BF16),
        ],
        1,
    )
    product = jnp.dot(all_gained, up_rel, preferred_element_type=F32).astype(BF16)
    sent = jnp.concatenate([product.reshape(4, 64, 1024), extra], 1)
    here = lax.axis_index("y")
    total = lax.dynamic_index_in_dim(sent, here, 0, keepdims=False).astype(F32)
    for d in (2, 1, 3):
        piece = lax.dynamic_index_in_dim(sent, (here + d) % 4, 0, keepdims=False)
        came = lax.ppermute(piece, "y", [(i, (i + d) % 4) for i in range(4)])
        total = total + came.astype(F32)
    sums = total[65, :384].reshape(3, 2, 64).sum(0)
    mean = sums[0] / 4096
    inverse = lax.rsqrt(sums[1] / 4096 - mean * mean + EPS)
    upward = (total[:64] - mean[:, None] * total[64:65]) * inverse[:, None]
    active = jnp.square(jax.nn.relu(upward)).astype(BF16)
    stat_parts = jnp.stack(apart(jnp.stack([mean, inverse]))).reshape(1, 384)
    block = jnp.concatenate(
        [active, jnp.pad(stat_parts, ((0, 7), (0, 640)))]
    )
    came = jnp.zeros((4, 72, 1024), BF16)
    came = lax.dynamic_update_index_in_dim(came, block, here, 0)
    for d in (2, 1, 3):
        piece = lax.ppermute(block, "y", [(i, (i + d) % 4) for i in range(4)])
        came = lax.dynamic_update_index_in_dim(came, piece, (here - d) % 4, 0)
    downward = scatter_tp(
        jnp.dot(came[:, :64].reshape(256, 1024), down_rel, preferred_element_type=F32)
    )
    stats = came[:, 64, :384].astype(F32).reshape(4, 3, 2, 64).sum(1)
    stats = stats.swapaxes(0, 1).reshape(2, 16, 16)
    index = lax.axis_index("c") * 8 + lax.axis_index("z")
    mean, inverse = lax.dynamic_index_in_dim(stats, index, 1, keepdims=False)
    hidden = (gained.astype(F32) - mean[:, None] * gain_rel[None]) * inverse[:, None]
    last = ALPHA * hidden + downward

    sums = jnp.stack([last.sum(1), (last * last).sum(1)], 1)
    sum_parts = jnp.concatenate(apart(sums), 1)
    pieces = rolled(last.astype(BF16).reshape(16, 4, 256).swapaxes(0, 1), (4 - place) % 4)
    sums_sent = jnp.broadcast_to(jnp.pad(sum_parts, ((0, 0), (0, 122)))[None], (4, 16, 128))
    came = lax.all_to_all(
        to_peers(jnp.concatenate([pieces, sums_sent], 2)), KV_ROWS, 0, 0, tiled=True
    )
    last = own_y(came[:, :, :256]).reshape(64, 256).astype(F32)
    sums = came[:, :, 256:262].astype(F32).reshape(2, 4, 2, 16, 3, 2).sum((1, 4))
    sums = sums.swapaxes(0, 1).reshape(64, 2)
    mean = sums[:, 0] / 4096
    inverse = lax.rsqrt(sums[:, 1] / 4096 - mean * mean + EPS)
    return ((last - mean[:, None]) * inverse[:, None] * final_gain[None]).astype(BF16)


def solution(mesh):
    finer = Mesh(mesh.devices.reshape(4, 2, 2, 8, 2), ("y", "xh", "xl", "z", "c"))
    placed = (
        P(TP, KV),
        P(KV),
        P(KV, None, TP),
        P(KV, None, TP),
        P(KV, None, TP),
        P(KV, TP),
        P(KV, TP),
        P(KV, TP),
        P(KV, TP),
        P(TP),
        P(TP),
        P(TP, KV),
        P(KV),
        P(KV, TP),
        P(TP, KV),
        P(KV),
    )

    return jax.shard_map(per_device, mesh=finer, in_specs=placed, out_specs=P(TP, KV), check_vma=False)
```

```python
import jax
import jax.numpy as jnp
from jax import lax
from jax.experimental import pallas as pl
from jax.experimental.layout import Layout, with_layout_constraint
from jax.experimental.pallas import tpu as pltpu
from jax.sharding import Mesh
from jax.sharding import PartitionSpec as P

HDIM = 64
BLK = 128
KV = ("y", "xh", "xl")
KV_ROWS = ("xl", "y", "xh")
TP = ("z", "c")
X = ("xh", "xl")

ALPHA = 2.0**0.5
EPS = 1e-05
F32 = jnp.float32
BF16 = jnp.bfloat16


def copy_for_each(x, axis):
    peers = lax.axis_size(axis)
    return lax.all_to_all(jnp.broadcast_to(x[None], (peers, *x.shape)), axis, 0, 0, tiled=True)


def gather_tp(x):
    parts = copy_for_each(x, "z")
    both = lax.all_gather(parts, "c", tiled=False)
    return both.reshape(-1, x.shape[1])


def scatter_tp(x):
    n = x.shape[1]
    halves = x.reshape(2, -1, n)
    core = lax.axis_index("c")
    mine = lax.dynamic_index_in_dim(halves, core, 0, keepdims=False)
    other = lax.dynamic_index_in_dim(halves, 1 - core, 0, keepdims=False).astype(BF16)
    arrived = lax.ppermute(other, "c", [(0, 1), (1, 0)])
    pair = (mine + arrived.astype(F32)).astype(BF16)
    parts = lax.all_to_all(pair.reshape(8, -1, n), "z", 0, 0, tiled=True)
    return parts.astype(F32).sum(axis=0)


def apart(x):
    high = lax.reduce_precision(x, 8, 7)
    rest = x - high
    middle = lax.reduce_precision(rest, 8, 7)
    return high.astype(BF16), middle.astype(BF16), (rest - middle).astype(BF16)


def rolled(x, start):
    return lax.dynamic_slice_in_dim(jnp.concatenate([x, x]), start, 4)


def to_peers(x):
    rest = x.shape[1:]
    x = x.reshape(2, 2, *rest).swapaxes(0, 1)
    return jnp.broadcast_to(x[:, None], (2, 4, 2, *rest)).reshape(16, *rest)


def own_y(x):
    rest = x.shape[1:]
    x = x.reshape(2, 4, 2, *rest)
    x = lax.dynamic_index_in_dim(x, lax.axis_index("y"), 1, keepdims=False)
    return x.swapaxes(0, 1).reshape(4, *rest)


def copied(kernel, out_shape, copies, limit, *args):
    many = isinstance(out_shape, tuple)
    vmem = pl.BlockSpec(memory_space=pltpu.VMEM)
    return pl.pallas_call(
        kernel,
        out_shape=out_shape,
        in_specs=[pl.BlockSpec(memory_space=pl.ANY)] * len(args),
        out_specs=(vmem,) * len(out_shape) if many else vmem,
        scratch_shapes=[pltpu.SemaphoreType.DMA((copies,))],
        compiler_params=pltpu.CompilerParams(vmem_limit_bytes=limit),
    )(*args)


def run_copies(pairs, sems):
    started = [
        pltpu.make_async_copy(source, target, sems.at[i]) for i, (source, target) in enumerate(pairs)
    ]
    for one in started:
        one.start()
    for one in started:
        one.wait()


def stack_kernel(own, after, far, before, stacked, sems):
    parts = (own, after, far, before)
    run_copies([(p, stacked.at[pl.ds(256 * i, 256)]) for i, p in enumerate(parts)], sems)


def beside_kernel(own, after, far, before, joined, sems):
    parts = (own, after, far, before)
    run_copies([(p, joined.at[:, pl.ds(256 * i, 256)]) for i, p in enumerate(parts)], sems)


def out_kernel(own, after, far, before, joined, gain):
    for i, p in enumerate((own, after, far, before)):
        lanes = pl.ds(256 * i, 256)
        joined[:, lanes] = p[:128]
        gain[:, lanes] = p[128:131].astype(F32).sum(0, keepdims=True)


def x_slots(x, far_back=False):
    forward = [(i, (i + 1) % 4) for i in range(4)]
    back = [(i, (i + 3) % 4) for i in range(4)]
    before = lax.ppermute(x, X, forward)
    after = lax.ppermute(x, X, back)
    far = lax.ppermute(after, X, back) if far_back else lax.ppermute(before, X, forward)
    return x, after, far, before


def head_sum(x):
    sums = [x[:, :HDIM].sum(1, keepdims=True), x[:, HDIM:].sum(1, keepdims=True)]
    return jnp.where(lax.broadcasted_iota(jnp.int32, x.shape, 1) < HDIM, *sums)


def retain_kernel(
    came, angles, heads, matrices, tokens, keys, values_from, state_from, sent, values, state, sems
):
    groups = []
    for i in range(4):
        rows = pl.ds(16 * i, 16)
        pairs = ((values_from, values), (state_from, state))
        groups.append(
            [
                pltpu.make_async_copy(source.at[rows], target.at[rows], sems.at[i, j])
                for j, (source, target) in enumerate(pairs)
            ]
        )
    for group in groups:
        for copy in group:
            copy.start()
    cosine, sine, offset = [angles[:, 128 * i : 128 * i + 128] for i in range(3)]
    rate, gain = heads[0:1], heads[1:2]
    swap, ones = matrices[:128], matrices[128:]

    summed = came[...].astype(F32).sum(0).astype(BF16)
    query, keyed, valued, gated = [summed[:, 128 * i : 128 * i + 128] for i in range(4)]

    def rotated(u):
        swapped = jnp.dot(u, swap, preferred_element_type=F32)
        return u.astype(F32) * cosine + swapped * sine

    q_short = rotated(query).astype(BF16)
    q_rot = q_short.astype(F32)
    k_rot = (rotated(keyed) * 0.125).astype(BF16).astype(F32)
    own = head_sum(q_rot * k_rot).astype(BF16).astype(F32)
    slot = lax.broadcasted_iota(jnp.int32, (BLK, 128), 0).astype(F32)
    growth = jnp.exp(rate * slot)
    key_index = lax.broadcasted_iota(jnp.int32, (HDIM, 128), 0)
    same = key_index == lax.broadcasted_iota(jnp.int32, (HDIM, 128), 1) % HDIM
    same = jnp.where(same, 1.0, 0.0).astype(BF16)
    inner, cross = [], []
    for s in range(64):
        if s % 16 == 0:
            for copy in groups[s // 16]:
                copy.wait()
        row = q_short[s : s + 1]
        terms = jnp.concatenate([keys[s] * row, same * row])
        spread = jnp.dot(terms, ones, preferred_element_type=F32)
        weights = jnp.where(slot < offset[s : s + 1], spread[:BLK] * growth, 0.0)
        inner.append((weights * values[s].astype(F32)).sum(0, keepdims=True))
        cross.append((spread[BLK:] * state[s]).sum(0, keepdims=True))
    inner = jnp.concatenate(inner) * jnp.exp(-rate * offset)
    cross = jnp.concatenate(cross) * jnp.exp(-rate * (offset + 1.0))
    retained = inner + own * valued.astype(F32) + cross
    centred = retained - head_sum(retained) / HDIM
    variance = head_sum(centred * centred) / HDIM
    normed = centred * lax.rsqrt(variance + EPS) * gain
    mixed = (jax.nn.silu(gated.astype(F32)) * normed).astype(BF16)
    for x in range(4):
        rows = pl.ds(16 * x, 16)
        for y in range(4):
            sent[x % 2, y, x // 2, :, :128] = mixed[16 * x : 16 * x + 16]
            sent[x % 2, y, x // 2, :, 128:] = tokens[rows]


def retain(came, lengths, state, keys, values, rate, gain, tokens):
    lane = jnp.arange(384)
    inverse = 10000.0 ** (-(lane % 32).astype(F32) / 32)
    angle = lengths.astype(F32)[:, None] * inverse[None]
    sine = jnp.sin(angle) * jnp.where(lane % HDIM < 32, -1.0, 1.0)[None]
    offset = (lengths % BLK).astype(F32)[:, None]
    angles = jnp.where(lane < 128, jnp.cos(angle), jnp.where(lane < 256, sine, offset))
    lane = lane[:128]
    swap = (lane[:, None] == (lane ^ 32)[None]).astype(BF16)
    ones = (lane[:, None] // HDIM == lane[None] // HDIM).astype(BF16)
    arrays = (
        came,
        angles,
        jnp.stack([jnp.repeat(rate, HDIM), gain]),
        jnp.concatenate([swap, ones]),
        tokens,
    )
    sent = pl.pallas_call(
        retain_kernel,
        out_shape=jax.ShapeDtypeStruct((2, 4, 2, 16, 384), BF16),
        in_specs=[pl.BlockSpec(memory_space=pltpu.VMEM)] * 6
        + [pl.BlockSpec(memory_space=pl.ANY)] * 2,
        out_specs=pl.BlockSpec(memory_space=pltpu.VMEM),
        scratch_shapes=[
            pltpu.VMEM((64, BLK, 128), BF16),
            pltpu.VMEM((64, HDIM, 128), F32),
            pltpu.SemaphoreType.DMA((4, 2)),
        ],
        compiler_params=pltpu.CompilerParams(vmem_limit_bytes=52000000),
    )(*arrays, keys, values, state)
    return sent.reshape(16, 16, 384)


def per_device(
    tokens,
    lengths,
    state_block,
    cached_keys,
    cached_values,
    query_weight,
    key_weight,
    value_weight,
    gate_weight,
    decay_rate,
    head_gain,
    out_weight,
    mixer_gain,
    up_weight,
    down_weight,
    final_gain,
):
    joined = lax.optimization_barrier(
        jnp.concatenate([query_weight, key_weight, value_weight, gate_weight], 1)
    )
    all_rows = gather_tp(tokens)
    partial = jnp.dot(all_rows, joined, preferred_element_type=F32).astype(BF16)
    partial = with_layout_constraint(partial, Layout((0, 1)))
    came = lax.all_to_all(partial.reshape(16, 64, 512), KV_ROWS, 0, 0, tiled=True)
    sent = retain(
        came,
        lengths,
        state_block,
        cached_keys,
        cached_values,
        decay_rate,
        head_gain,
        tokens,
    )
    packed = jnp.concatenate(
        [out_weight, jnp.stack(apart(mixer_gain) + (jnp.zeros((256,), BF16),) * 5)]
    )
    out_slots = x_slots(packed)
    out_rel, gain_rel = pl.pallas_call(
        out_kernel,
        out_shape=(jax.ShapeDtypeStruct((128, 1024), BF16), jax.ShapeDtypeStruct((1, 1024), F32)),
        compiler_params=pltpu.CompilerParams(vmem_limit_bytes=4 * 2**20),
    )(*out_slots)
    gain_rel = gain_rel[0]
    square = jax.ShapeDtypeStruct((1024, 1024), BF16)
    up_slots = x_slots(up_weight)
    up_rel = copied(stack_kernel, square, 4, None, *up_slots)
    down_slots = x_slots(down_weight, far_back=True)
    down_rel = copied(beside_kernel, square, 4, None, *down_slots)
    place = lax.axis_index(X)

    came = lax.all_to_all(sent, KV_ROWS, 0, 0, tiled=True)
    mixed_rows = came[:, :, :128].reshape(256, 128)
    token_rows = rolled(own_y(came[:, :, 128:]), place).swapaxes(0, 1).reshape(16, 1024)

    partial = jnp.dot(mixed_rows, out_rel, preferred_element_type=F32)
    branch = scatter_tp(partial)
    values = ALPHA * token_rows.astype(F32) + branch
    gained = (values * gain_rel[None]).astype(BF16)
    all_gained = gather_tp(gained)

    plain = all_gained.astype(F32) / gain_rel[None]
    sums = jnp.stack([plain.sum(1).reshape(4, 64), (plain * plain).sum(1).reshape(4, 64)], 1)
    sum_parts = jnp.stack(apart(sums), 1).reshape(4, 1, 384)
    gain_row = jnp.dot(jnp.stack(apart(gain_rel)), up_rel, preferred_element_type=F32)
    gain_row = gain_row.sum(0, keepdims=True).astype(BF16)
    extra = jnp.concatenate(
        [
            jnp.broadcast_to(gain_row[None], (4, 1, 1024)),
            jnp.pad(sum_parts, ((0, 0), (0, 0), (0, 640))),
            jnp.zeros((4, 6, 1024), BF16),
        ],
        1,
    )
    product = jnp.dot(all_gained, up_rel, preferred_element_type=F32).astype(BF16)
    sent = jnp.concatenate([product.reshape(4, 64, 1024), extra], 1)
    here = lax.axis_index("y")
    total = lax.dynamic_index_in_dim(sent, here, 0, keepdims=False).astype(F32)
    for d in (2, 1, 3):
        piece = lax.dynamic_index_in_dim(sent, (here + d) % 4, 0, keepdims=False)
        came = lax.ppermute(piece, "y", [(i, (i + d) % 4) for i in range(4)])
        total = total + came.astype(F32)
    sums = total[65, :384].reshape(3, 2, 64).sum(0)
    mean = sums[0] / 4096
    inverse = lax.rsqrt(sums[1] / 4096 - mean * mean + EPS)
    upward = (total[:64] - mean[:, None] * total[64:65]) * inverse[:, None]
    active = jnp.square(jax.nn.relu(upward)).astype(BF16)
    stat_parts = jnp.stack(apart(jnp.stack([mean, inverse]))).reshape(1, 384)
    block = jnp.concatenate(
        [active, jnp.pad(stat_parts, ((0, 7), (0, 640)))]
    )
    came = jnp.zeros((4, 72, 1024), BF16)
    came = lax.dynamic_update_index_in_dim(came, block, here, 0)
    for d in (2, 1, 3):
        piece = lax.ppermute(block, "y", [(i, (i + d) % 4) for i in range(4)])
        came = lax.dynamic_update_index_in_dim(came, piece, (here - d) % 4, 0)
    downward = scatter_tp(
        jnp.dot(came[:, :64].reshape(256, 1024), down_rel, preferred_element_type=F32)
    )
    stats = came[:, 64, :384].astype(F32).reshape(4, 3, 2, 64).sum(1)
    stats = stats.swapaxes(0, 1).reshape(2, 16, 16)
    index = lax.axis_index("c") * 8 + lax.axis_index("z")
    mean, inverse = lax.dynamic_index_in_dim(stats, index, 1, keepdims=False)
    hidden = (gained.astype(F32) - mean[:, None] * gain_rel[None]) * inverse[:, None]
    last = ALPHA * hidden + downward

    sums = jnp.stack([last.sum(1), (last * last).sum(1)], 1)
    sum_parts = jnp.concatenate(apart(sums), 1)
    pieces = rolled(last.astype(BF16).reshape(16, 4, 256).swapaxes(0, 1), (4 - place) % 4)
    sums_sent = jnp.broadcast_to(jnp.pad(sum_parts, ((0, 0), (0, 122)))[None], (4, 16, 128))
    came = lax.all_to_all(
        to_peers(jnp.concatenate([pieces, sums_sent], 2)), KV_ROWS, 0, 0, tiled=True
    )
    last = own_y(came[:, :, :256]).reshape(64, 256).astype(F32)
    sums = came[:, :, 256:262].astype(F32).reshape(2, 4, 2, 16, 3, 2).sum((1, 4))
    sums = sums.swapaxes(0, 1).reshape(64, 2)
    mean = sums[:, 0] / 4096
    inverse = lax.rsqrt(sums[:, 1] / 4096 - mean * mean + EPS)
    return ((last - mean[:, None]) * inverse[:, None] * final_gain[None]).astype(BF16)


def solution(mesh):
    finer = Mesh(mesh.devices.reshape(4, 2, 2, 8, 2), ("y", "xh", "xl", "z", "c"))
    placed = (
        P(TP, KV),
        P(KV),
        P(KV, None, TP),
        P(KV, None, TP),
        P(KV, None, TP),
        P(KV, TP),
        P(KV, TP),
        P(KV, TP),
        P(KV, TP),
        P(TP),
        P(TP),
        P(TP, KV),
        P(KV),
        P(KV, TP),
        P(TP, KV),
        P(KV),
    )

    return jax.shard_map(per_device, mesh=finer, in_specs=placed, out_specs=P(TP, KV), check_vma=False)
```

```python
import jax
import jax.numpy as jnp
from jax import lax
from jax.experimental import pallas as pl
from jax.experimental.layout import Layout, with_layout_constraint
from jax.experimental.pallas import tpu as pltpu
from jax.sharding import Mesh
from jax.sharding import PartitionSpec as P

HDIM = 64
BLK = 128
KV = ("y", "xh", "xl")
KV_ROWS = ("xl", "y", "xh")
TP = ("z", "c")
X = ("xh", "xl")

ALPHA = 2.0**0.5
EPS = 1e-05
F32 = jnp.float32
BF16 = jnp.bfloat16


def copy_for_each(x, axis):
    peers = lax.axis_size(axis)
    return lax.all_to_all(jnp.broadcast_to(x[None], (peers, *x.shape)), axis, 0, 0, tiled=True)


def gather_tp(x):
    parts = copy_for_each(x, "z")
    both = lax.all_gather(parts, "c", tiled=False)
    return both.reshape(-1, x.shape[1])


def scatter_tp(x):
    n = x.shape[1]
    halves = x.reshape(2, -1, n)
    core = lax.axis_index("c")
    mine = lax.dynamic_index_in_dim(halves, core, 0, keepdims=False)
    other = lax.dynamic_index_in_dim(halves, 1 - core, 0, keepdims=False).astype(BF16)
    arrived = lax.ppermute(other, "c", [(0, 1), (1, 0)])
    pair = (mine + arrived.astype(F32)).astype(BF16)
    parts = lax.all_to_all(pair.reshape(8, -1, n), "z", 0, 0, tiled=True)
    return parts.astype(F32).sum(axis=0)


def apart(x):
    high = lax.reduce_precision(x, 8, 7)
    rest = x - high
    middle = lax.reduce_precision(rest, 8, 7)
    return high.astype(BF16), middle.astype(BF16), (rest - middle).astype(BF16)


def rolled(x, start):
    return lax.dynamic_slice_in_dim(jnp.concatenate([x, x]), start, 4)


def to_peers(x):
    rest = x.shape[1:]
    x = x.reshape(2, 2, *rest).swapaxes(0, 1)
    return jnp.broadcast_to(x[:, None], (2, 4, 2, *rest)).reshape(16, *rest)


def own_y(x):
    rest = x.shape[1:]
    x = x.reshape(2, 4, 2, *rest)
    x = lax.dynamic_index_in_dim(x, lax.axis_index("y"), 1, keepdims=False)
    return x.swapaxes(0, 1).reshape(4, *rest)


def copied(kernel, out_shape, copies, limit, *args):
    many = isinstance(out_shape, tuple)
    vmem = pl.BlockSpec(memory_space=pltpu.VMEM)
    return pl.pallas_call(
        kernel,
        out_shape=out_shape,
        in_specs=[pl.BlockSpec(memory_space=pl.ANY)] * len(args),
        out_specs=(vmem,) * len(out_shape) if many else vmem,
        scratch_shapes=[pltpu.SemaphoreType.DMA((copies,))],
        compiler_params=pltpu.CompilerParams(vmem_limit_bytes=limit),
    )(*args)


def run_copies(pairs, sems):
    started = [
        pltpu.make_async_copy(source, target, sems.at[i]) for i, (source, target) in enumerate(pairs)
    ]
    for one in started:
        one.start()
    for one in started:
        one.wait()


def stack_kernel(own, after, far, before, stacked, sems):
    parts = (own, after, far, before)
    run_copies([(p, stacked.at[pl.ds(256 * i, 256)]) for i, p in enumerate(parts)], sems)


def beside_kernel(own, after, far, before, joined, sems):
    parts = (own, after, far, before)
    run_copies([(p, joined.at[:, pl.ds(256 * i, 256)]) for i, p in enumerate(parts)], sems)


def out_kernel(own, after, far, before, joined, gain):
    for i, p in enumerate((own, after, far, before)):
        lanes = pl.ds(256 * i, 256)
        joined[:, lanes] = p[:128]
        gain[:, lanes] = p[128:131].astype(F32).sum(0, keepdims=True)


def x_slots(x, far_back=False):
    forward = [(i, (i + 1) % 4) for i in range(4)]
    back = [(i, (i + 3) % 4) for i in range(4)]
    before = lax.ppermute(x, X, forward)
    after = lax.ppermute(x, X, back)
    far = lax.ppermute(after, X, back) if far_back else lax.ppermute(before, X, forward)
    return x, after, far, before


def head_sum(x):
    sums = [x[:, :HDIM].sum(1, keepdims=True), x[:, HDIM:].sum(1, keepdims=True)]
    return jnp.where(lax.broadcasted_iota(jnp.int32, x.shape, 1) < HDIM, *sums)


def retain_kernel(
    came, angles, heads, matrices, keys, values_from, state_from, sent, values, state, sems
):
    groups = []
    for i in range(4):
        rows = pl.ds(16 * i, 16)
        pairs = ((values_from, values), (state_from, state))
        groups.append(
            [
                pltpu.make_async_copy(source.at[rows], target.at[rows], sems.at[i, j])
                for j, (source, target) in enumerate(pairs)
            ]
        )
    for group in groups:
        for copy in group:
            copy.start()
    cosine, sine, offset = [angles[:, 128 * i : 128 * i + 128] for i in range(3)]
    rate, gain = heads[0:1], heads[1:2]
    swap, ones = matrices[:128], matrices[128:]

    summed = came[...].astype(F32).sum(0).astype(BF16)
    query, keyed, valued, gated = [summed[:, 128 * i : 128 * i + 128] for i in range(4)]

    def rotated(u):
        swapped = jnp.dot(u, swap, preferred_element_type=F32)
        return u.astype(F32) * cosine + swapped * sine

    q_short = rotated(query).astype(BF16)
    q_rot = q_short.astype(F32)
    k_rot = (rotated(keyed) * 0.125).astype(BF16).astype(F32)
    own = head_sum(q_rot * k_rot).astype(BF16).astype(F32)
    slot = lax.broadcasted_iota(jnp.int32, (BLK, 128), 0).astype(F32)
    growth = jnp.exp(rate * slot)
    key_index = lax.broadcasted_iota(jnp.int32, (HDIM, 128), 0)
    same = key_index == lax.broadcasted_iota(jnp.int32, (HDIM, 128), 1) % HDIM
    same = jnp.where(same, 1.0, 0.0).astype(BF16)
    inner, cross = [], []
    for s in range(64):
        if s % 16 == 0:
            for copy in groups[s // 16]:
                copy.wait()
        row = q_short[s : s + 1]
        terms = jnp.concatenate([keys[s] * row, same * row])
        spread = jnp.dot(terms, ones, preferred_element_type=F32)
        weights = jnp.where(slot < offset[s : s + 1], spread[:BLK] * growth, 0.0)
        inner.append((weights * values[s].astype(F32)).sum(0, keepdims=True))
        cross.append((spread[BLK:] * state[s]).sum(0, keepdims=True))
    inner = jnp.concatenate(inner) * jnp.exp(-rate * offset)
    cross = jnp.concatenate(cross) * jnp.exp(-rate * (offset + 1.0))
    retained = inner + own * valued.astype(F32) + cross
    centred = retained - head_sum(retained) / HDIM
    variance = head_sum(centred * centred) / HDIM
    normed = centred * lax.rsqrt(variance + EPS) * gain
    mixed = (jax.nn.silu(gated.astype(F32)) * normed).astype(BF16)
    for x in range(4):
        for y in range(4):
            sent[x % 2, y, x // 2] = mixed[16 * x : 16 * x + 16]


def retain(came, lengths, state, keys, values, rate, gain):
    lane = jnp.arange(384)
    inverse = 10000.0 ** (-(lane % 32).astype(F32) / 32)
    angle = lengths.astype(F32)[:, None] * inverse[None]
    sine = jnp.sin(angle) * jnp.where(lane % HDIM < 32, -1.0, 1.0)[None]
    offset = (lengths % BLK).astype(F32)[:, None]
    angles = jnp.where(lane < 128, jnp.cos(angle), jnp.where(lane < 256, sine, offset))
    lane = lane[:128]
    swap = (lane[:, None] == (lane ^ 32)[None]).astype(BF16)
    ones = (lane[:, None] // HDIM == lane[None] // HDIM).astype(BF16)
    arrays = (
        came,
        angles,
        jnp.stack([jnp.repeat(rate, HDIM), gain]),
        jnp.concatenate([swap, ones]),
    )
    sent = pl.pallas_call(
        retain_kernel,
        out_shape=jax.ShapeDtypeStruct((2, 4, 2, 16, 128), BF16),
        in_specs=[pl.BlockSpec(memory_space=pltpu.VMEM)] * 5
        + [pl.BlockSpec(memory_space=pl.ANY)] * 2,
        out_specs=pl.BlockSpec(memory_space=pltpu.VMEM),
        scratch_shapes=[
            pltpu.VMEM((64, BLK, 128), BF16),
            pltpu.VMEM((64, HDIM, 128), F32),
            pltpu.SemaphoreType.DMA((4, 2)),
        ],
        compiler_params=pltpu.CompilerParams(vmem_limit_bytes=52000000),
    )(*arrays, keys, values, state)
    return sent.reshape(16, 16, 128)


def per_device(
    tokens,
    lengths,
    state_block,
    cached_keys,
    cached_values,
    query_weight,
    key_weight,
    value_weight,
    gate_weight,
    decay_rate,
    head_gain,
    out_weight,
    mixer_gain,
    up_weight,
    down_weight,
    final_gain,
):
    joined = lax.optimization_barrier(
        jnp.concatenate([query_weight, key_weight, value_weight, gate_weight], 1)
    )
    all_rows = gather_tp(tokens)
    partial = jnp.dot(all_rows, joined, preferred_element_type=F32).astype(BF16)
    partial = with_layout_constraint(partial, Layout((0, 1)))
    came = lax.all_to_all(partial.reshape(16, 64, 512), KV_ROWS, 0, 0, tiled=True)
    sent = retain(
        came,
        lengths,
        state_block,
        cached_keys,
        cached_values,
        decay_rate,
        head_gain,
    )
    packed = jnp.concatenate(
        [out_weight, jnp.stack(apart(mixer_gain) + (jnp.zeros((256,), BF16),) * 5)]
    )
    out_slots = x_slots(packed)
    out_rel, gain_rel = pl.pallas_call(
        out_kernel,
        out_shape=(jax.ShapeDtypeStruct((128, 1024), BF16), jax.ShapeDtypeStruct((1, 1024), F32)),
        compiler_params=pltpu.CompilerParams(vmem_limit_bytes=4 * 2**20),
    )(*out_slots)
    gain_rel = gain_rel[0]
    square = jax.ShapeDtypeStruct((1024, 1024), BF16)
    up_slots = x_slots(up_weight)
    up_rel = copied(stack_kernel, square, 4, None, *up_slots)
    down_slots = x_slots(down_weight, far_back=True)
    down_rel = copied(beside_kernel, square, 4, None, *down_slots)
    place = lax.axis_index(X)

    came = lax.all_to_all(sent, KV_ROWS, 0, 0, tiled=True)
    mixed_rows = came.reshape(256, 128)
    quarters = tokens.reshape(4, 16, 256)
    token_slots = [lax.dynamic_index_in_dim(quarters, place, 0, keepdims=False)]
    for d in (3, 2, 1):
        piece = lax.dynamic_index_in_dim(quarters, (place + d) % 4, 0, keepdims=False)
        came = lax.ppermute(piece, X, [(i, (i + d) % 4) for i in range(4)])
        token_slots.append(came)
    token_rows = jnp.concatenate(token_slots, 1)

    partial = jnp.dot(mixed_rows, out_rel, preferred_element_type=F32)
    branch = scatter_tp(partial)
    values = ALPHA * token_rows.astype(F32) + branch
    gained = (values * gain_rel[None]).astype(BF16)
    all_gained = gather_tp(gained)

    plain = all_gained.astype(F32) / gain_rel[None]
    sums = jnp.stack([plain.sum(1).reshape(4, 64), (plain * plain).sum(1).reshape(4, 64)], 1)
    sum_parts = jnp.stack(apart(sums), 1).reshape(4, 1, 384)
    gain_row = jnp.dot(jnp.stack(apart(gain_rel)), up_rel, preferred_element_type=F32)
    gain_row = gain_row.sum(0, keepdims=True).astype(BF16)
    extra = jnp.concatenate(
        [
            jnp.broadcast_to(gain_row[None], (4, 1, 1024)),
            jnp.pad(sum_parts, ((0, 0), (0, 0), (0, 640))),
            jnp.zeros((4, 6, 1024), BF16),
        ],
        1,
    )
    product = jnp.dot(all_gained, up_rel, preferred_element_type=F32).astype(BF16)
    sent = jnp.concatenate([product.reshape(4, 64, 1024), extra], 1)
    here = lax.axis_index("y")
    total = lax.dynamic_index_in_dim(sent, here, 0, keepdims=False).astype(F32)
    for d in (2, 1, 3):
        piece = lax.dynamic_index_in_dim(sent, (here + d) % 4, 0, keepdims=False)
        came = lax.ppermute(piece, "y", [(i, (i + d) % 4) for i in range(4)])
        total = total + came.astype(F32)
    sums = total[65, :384].reshape(3, 2, 64).sum(0)
    mean = sums[0] / 4096
    inverse = lax.rsqrt(sums[1] / 4096 - mean * mean + EPS)
    upward = (total[:64] - mean[:, None] * total[64:65]) * inverse[:, None]
    active = jnp.square(jax.nn.relu(upward)).astype(BF16)
    everyone = jnp.zeros((4, 64, 1024), BF16)
    everyone = lax.dynamic_update_index_in_dim(everyone, active, here, 0)
    for d in (2, 1, 3):
        piece = lax.ppermute(active, "y", [(i, (i + d) % 4) for i in range(4)])
        everyone = lax.dynamic_update_index_in_dim(everyone, piece, (here - d) % 4, 0)
    partial = jnp.dot(everyone.reshape(256, 1024), down_rel, preferred_element_type=F32)
    downward = scatter_tp(partial)
    own_stats = jnp.pad(
        jnp.stack(apart(jnp.stack([mean, inverse]))).reshape(3, 128), ((0, 5), (0, 0))
    )
    stats = jnp.zeros((4, 8, 128), BF16)
    stats = lax.dynamic_update_index_in_dim(stats, own_stats, here, 0)
    for d in (2, 1, 3):
        piece = lax.ppermute(own_stats, "y", [(i, (i + d) % 4) for i in range(4)])
        stats = lax.dynamic_update_index_in_dim(stats, piece, (here - d) % 4, 0)
    stats = stats[:, :3].astype(F32).sum(1).reshape(4, 2, 64)
    stats = stats.swapaxes(0, 1).reshape(2, 16, 16)
    index = lax.axis_index("c") * 8 + lax.axis_index("z")
    mean, inverse = lax.dynamic_index_in_dim(stats, index, 1, keepdims=False)
    hidden = (gained.astype(F32) - mean[:, None] * gain_rel[None]) * inverse[:, None]
    last = ALPHA * hidden + downward

    sums = jnp.stack([last.sum(1), (last * last).sum(1)], 1)
    sum_parts = jnp.concatenate(apart(sums), 1)
    pieces = rolled(last.astype(BF16).reshape(16, 4, 256).swapaxes(0, 1), (4 - place) % 4)
    sums_sent = jnp.broadcast_to(jnp.pad(sum_parts, ((0, 0), (0, 122)))[None], (4, 16, 128))
    came = lax.all_to_all(
        to_peers(jnp.concatenate([pieces, sums_sent], 2)), KV_ROWS, 0, 0, tiled=True
    )
    last = own_y(came[:, :, :256]).reshape(64, 256).astype(F32)
    sums = came[:, :, 256:262].astype(F32).reshape(2, 4, 2, 16, 3, 2).sum((1, 4))
    sums = sums.swapaxes(0, 1).reshape(64, 2)
    mean = sums[:, 0] / 4096
    inverse = lax.rsqrt(sums[:, 1] / 4096 - mean * mean + EPS)
    return ((last - mean[:, None]) * inverse[:, None] * final_gain[None]).astype(BF16)


def solution(mesh):
    finer = Mesh(mesh.devices.reshape(4, 2, 2, 8, 2), ("y", "xh", "xl", "z", "c"))
    placed = (
        P(TP, KV),
        P(KV),
        P(KV, None, TP),
        P(KV, None, TP),
        P(KV, None, TP),
        P(KV, TP),
        P(KV, TP),
        P(KV, TP),
        P(KV, TP),
        P(TP),
        P(TP),
        P(TP, KV),
        P(KV),
        P(KV, TP),
        P(TP, KV),
        P(KV),
    )

    return jax.shard_map(per_device, mesh=finer, in_specs=placed, out_specs=P(TP, KV), check_vma=False)
```
